512 devices in a mesh: tp: 16 (over y, x), dp: 32 (over z, core).
Axes of the slice: x: 4, y: 4, z: 16, core: 2. Of those that a mesh axis runs over, the one named last changes fastest.
Arguments:
- tokens: bfloat16 [256, 4096], P('tp', 'dp'), may hold values from -12 to 12, as said below
- norm_gain: float32 [2, 4096], P(None, 'dp'), may hold values from 0.1 to 1.9
- w_input: bfloat16 [2, 4096, 2048], P(None, 'dp', 'tp'), may hold values from -0.09375 to 0.09375
- w_gate: bfloat16 [2, 4096, 2048], P(None, 'dp', 'tp'), may hold values from -0.09375 to 0.09375
- w_recur: bfloat16 [2, 16, 128, 128], P(None, 'tp'), may hold values from -0.5 to 0.5
- w_inject: bfloat16 [2, 16, 128, 128], P(None, 'tp'), may hold values from -0.5 to 0.5
- conv_weight: bfloat16 [2, 4, 2048], P(None, None, 'tp'), may hold values from -3 to 3
- decay_param: float32 [2, 2048], P(None, 'tp'), may hold values from -2 to 5
- w_output: bfloat16 [2, 2048, 4096], P(None, 'tp', 'dp'), may hold values from -0.125 to 0.125
- lengths: int32 [256], P('dp'), may hold values from 1 to 48, 2048 in all
- conv_state: bfloat16 [2, 3, 256, 2048], P(None, None, 'dp', 'tp'), may hold values from -6 to 6
- rec_state: float32 [2, 256, 2048], P(None, 'dp', 'tp'), may hold values from -6 to 6
Outputs:
- mixed: bfloat16 [256, 4096], P('tp', 'dp')
- new_conv: bfloat16 [2, 3, 256, 2048], P(None, None, 'dp', 'tp')
- new_rec: float32 [2, 256, 2048], P(None, 'dp', 'tp')
The draws below stay inside these ranges and needn't reach their ends.
Inputs may be any that keep to these rules, and one draw needn't show every extreme that they name: `tokens`: activations; feature scales vary.
All inputs are finite; a program needn't handle non-finite values. No bound on the sum of `lengths` on one device may be relied on, other than what follows from the above.
Results may differ from the reference program's by a relative error of at most 0.02.
Values may be sent and summed in bfloat16 or wider, within the bound.
A program may use at most 64 MiB of HBM per device.

```python
import math
import jax
import jax.numpy as jnp
import numpy as np
from jax import lax

D = 4096
NB = 16
BLK = 128
CONV = 4
W = 2048
BATCH = 256


def draw_tokens(key, part):
    col_scale = jnp.exp(jnp.linspace(jnp.log(0.5), jnp.log(2.0), D)).astype(jnp.float32)
    values = jnp.clip(jax.random.normal(key, (BATCH, D), jnp.float32), -6.0, 6.0)
    return (values * col_scale).astype(jnp.bfloat16)


def block_levels(key, extent, shards, low, high):
    def one(dim, parts):
        heights = jax.random.uniform(jax.random.fold_in(jax.random.fold_in(key, 6), dim), (parts,), jnp.float32, low / len(shards), high / len(shards))
        return jnp.repeat(jnp.exp(heights), extent[dim] // parts).reshape((-1,) + (1,) * (len(extent) - dim - 1))

    gain = one(*shards[0])
    for cut in shards[1:]:
        gain = gain * one(*cut)
    return gain


def split_up(count, total, reach, slope):
    weights = [(1 << 20) // math.isqrt(grade ** slope) + 1 for grade in range(2, count + 1)]
    surplus, holding = total - reach - (count - 1), [1] * (count - 1)
    while surplus > 0:
        movable = [i for i in range(count - 1) if holding[i] < reach]
        pool, left = sum([weights[i] for i in movable]), surplus
        for i in movable:
            addition = min(reach - holding[i], max(1, left * weights[i] // pool), surplus)
            holding[i] = holding[i] + addition
            surplus = surplus - addition
    return np.array([reach] + holding)


def uneven_parts(own_key, count, total, reach, slope):
    if count == 2:
        one = jax.random.randint(own_key, (), max(1, total - reach), min(reach, total - 1) + 1)
        return jnp.stack([one, total - one])
    sizes = jnp.asarray(split_up(count, total, reach, slope), jnp.int32)
    couples = (count - 1) // 2
    source_of, receiver = sizes[1:1 + 2 * couples:2], sizes[2:2 + 2 * couples:2]
    slack = jnp.minimum(source_of - 1, reach - receiver)
    shifted = jax.random.randint(jax.random.fold_in(own_key, 1), (couples,), 0, 1 << 20) % (slack + 1)
    sizes = sizes.at[1:1 + 2 * couples:2].set(source_of - shifted).at[2:2 + 2 * couples:2].set(receiver + shifted)
    return sizes[jax.random.permutation(jax.random.fold_in(own_key, 2), count)]


def bell_draw(key, dims, deviation, most, cuts=(), dtype=jnp.bfloat16):
    gain = block_levels(key, dims, cuts, -0.22, 0.18) if cuts else 1.0
    array = jax.random.normal(key, dims, jnp.float32) * deviation * gain
    return jnp.minimum(jnp.maximum(array, -most), most).astype(dtype)


def setup_inputs(seed: int = 0) -> dict:
    streams_of = jax.random.split(jax.random.key(seed), 13)
    return {
        "tokens": draw_tokens(jax.random.fold_in(streams_of[12], 71), 0),
        "norm_gain": jnp.clip(1.0 + 0.18 * jax.random.normal(streams_of[1], (2, D), jnp.float32), 0.1, 1.9),
        "w_input": bell_draw(streams_of[2], (2, D, W), D ** -0.5, 0.09375, ((1, 32), (2, 16))),
        "w_gate": bell_draw(streams_of[3], (2, D, W), D ** -0.5, 0.09375, ((1, 32), (2, 16))),
        "w_recur": bell_draw(streams_of[4], (2, NB, BLK, BLK), BLK ** -0.5, 0.5, ((1, 16),)),
        "w_inject": bell_draw(streams_of[5], (2, NB, BLK, BLK), BLK ** -0.5, 0.5, ((1, 16),)),
        "conv_weight": bell_draw(streams_of[6], (2, CONV, W), CONV ** -0.5, 3.0, ((2, 16),)),
        "decay_param": jnp.clip(-2.0 + 7.0 * jax.random.uniform(streams_of[7], (2, W), jnp.float32) ** block_levels(streams_of[7], (2, W), ((1, 16),), -0.2, 0.2), -2.0, 5.0),
        "w_output": bell_draw(streams_of[8], (2, W, D), W ** -0.5, 0.125, ((1, 16), (2, 32))),
        "lengths": uneven_parts(streams_of[9], BATCH, 8 * BATCH, 48, 2).astype(jnp.int32),
        "conv_state": bell_draw(streams_of[10], (2, CONV - 1, BATCH, W), 1.0, 6.0, ((2, 32), (3, 16))),
        "rec_state": bell_draw(streams_of[11], (2, BATCH, W), 1.0, 6.0, ((1, 32), (2, 16)), jnp.float32),
    }


EPS = 1e-06

def reference(tokens, norm_gain, w_input, w_gate, w_recur, w_inject, conv_weight, decay_param, w_output, lengths, conv_state, rec_state):
    current = tokens
    live_len = lengths[:, None]
    conv_list = []
    rec_list = []
    for layer_idx in range(2):
        widened = current.astype(jnp.float32)
        rscale = lax.rsqrt(lax.optimization_barrier(jnp.mean(widened * widened, axis=1, keepdims=True)) + EPS)
        scaled = (widened * norm_gain[layer_idx]).astype(jnp.bfloat16)
        value_in = jnp.dot(scaled, w_input[layer_idx], preferred_element_type=jnp.float32) * rscale
        gate_in = jnp.dot(scaled, w_gate[layer_idx], preferred_element_type=jnp.float32) * rscale
        conv_taps = conv_weight[layer_idx].astype(jnp.float32)
        old_taps = conv_state[layer_idx]
        tap_count = old_taps.shape[0]
        conv_out = conv_taps[tap_count] * value_in
        for back in range(1, tap_count + 1):
            conv_out = conv_out + conv_taps[tap_count - back] * jnp.where(back < live_len, old_taps[tap_count - back].astype(jnp.float32), jnp.float32(0.0))
        conv_low = conv_out.astype(jnp.bfloat16).reshape(BATCH, NB, BLK).astype(jnp.float32)
        rec_gate = jax.nn.sigmoid(jnp.einsum('bnc,ncd->bnd', conv_low, w_recur[layer_idx].astype(jnp.float32)).reshape(BATCH, W))
        inp_gate = jax.nn.sigmoid(jnp.einsum('bnc,ncd->bnd', conv_low, w_inject[layer_idx].astype(jnp.float32)).reshape(BATCH, W))
        log_decay = -8.0 * rec_gate * jax.nn.softplus(-decay_param[layer_idx])
        previous = jnp.where(live_len > 1, rec_state[layer_idx], jnp.float32(0.0))
        hidden = jnp.exp(log_decay) * previous + jnp.sqrt(-jnp.expm1(2.0 * log_decay)) * (inp_gate * conv_out)
        readout = (hidden * jax.nn.gelu(gate_in)).astype(jnp.bfloat16)
        current = (widened + jnp.dot(readout, w_output[layer_idx], preferred_element_type=jnp.float32)).astype(jnp.bfloat16)
        conv_list.append(jnp.concatenate([old_taps[1:], value_in.astype(jnp.bfloat16)[None]], axis=0))
        rec_list.append(hidden)
    return (current, jnp.stack(conv_list), jnp.stack(rec_list))
```

```python
import functools

import jax
import jax.numpy as jnp
from jax import lax
from jax.experimental import pallas as pl
from jax.experimental.pallas import tpu as pltpu
from jax.sharding import PartitionSpec as P

EPS = 1e-06
MESH = pl.DeviceIdType.MESH
BF = jnp.bfloat16
F32 = jnp.float32
LN = 128


def tp_peer(nt, me, j):
    if nt != 16:
        return lax.rem(me + j + 1, nt)
    i = j + j // 10
    y = (me // 4 + 2 + i // 4) % 4
    x = (me + 2 + i % 4) % 4
    return y * 4 + x


def dp_peer(nd, me, j):
    nz = nd // 2
    i = j // 2
    z = (me // 2 + nz // 2 + ((i + 1) // 2) * (2 * (i % 2) - 1) + nz) % nz
    return z * 2 + j % 2


def one_less_exp(y):
    near = -y * (1.0 + y * (1 / 2 + y * (1 / 6 + y * (1 / 24 + y * (1 / 120)))))
    return jnp.where(y > -0.1, near, 1.0 - jnp.exp(y))


def kernel(nt, nd, tr, sr, lens, tok, gain, win, wgate, wrec, winj, cw, dec, wout, cs, rs,
           mixed, nconv, nrec,
           x_v, gain_v, wcat, rcat, cw_v, dec_v, wout_v, cs_v, rs_v,
           xg, pb, rb, ssb, ssr, ro, rg, ob, og, x1, nconv_v, nrec_v,
           ssem, rsem, lsem, osem):
    t = lax.axis_index("tp")
    d = lax.axis_index("dp")
    nr = nt * tr
    width = nd * LN

    loads = [
        pltpu.make_async_copy(tok, x_v, lsem.at[0]),
        pltpu.make_async_copy(gain, gain_v, lsem.at[1]),
        pltpu.make_async_copy(win, wcat.at[:, :, pl.ds(0, LN)], lsem.at[2]),
        pltpu.make_async_copy(wgate, wcat.at[:, :, pl.ds(LN, LN)], lsem.at[3]),
        pltpu.make_async_copy(wrec.at[:, 0], rcat.at[:, :, pl.ds(0, LN)], lsem.at[4]),
        pltpu.make_async_copy(winj.at[:, 0], rcat.at[:, :, pl.ds(LN, LN)], lsem.at[5]),
        pltpu.make_async_copy(cw, cw_v, lsem.at[6]),
        pltpu.make_async_copy(dec, dec_v, lsem.at[7]),
        pltpu.make_async_copy(wout, wout_v, lsem.at[8]),
        pltpu.make_async_copy(cs, cs_v, lsem.at[9]),
        pltpu.make_async_copy(rs, rs_v, lsem.at[10]),
    ]
    for c in loads:
        c.start()

    barrier = pltpu.get_barrier_semaphore()

    def sig_dp(j, _):
        pl.semaphore_signal(barrier, inc=1, device_id={"dp": dp_peer(nd, d, j)}, device_id_type=MESH)
        return 0

    def sig_tp(j, _):
        pl.semaphore_signal(barrier, inc=1, device_id={"tp": tp_peer(nt, t, j)}, device_id_type=MESH)
        return 0

    lax.fori_loop(0, nd - 2, sig_dp, 0)
    pl.semaphore_signal(barrier, inc=1, device_id={"dp": d + 1 - 2 * (d % 2)}, device_id_type=MESH)
    lax.fori_loop(0, nt - 1, sig_tp, 0)
    pl.semaphore_wait(barrier, nt + nd - 2)

    def remote(src, dst, s, dev):
        return pltpu.make_async_remote_copy(
            src_ref=src, dst_ref=dst, send_sem=ssem.at[s], recv_sem=rsem.at[s],
            device_id=dev, device_id_type=MESH)

    def send_tp(src_of, dst, s):
        def step(j, _):
            p = tp_peer(nt, t, j)
            remote(src_of(p), dst, s, {"tp": p}).start()
            return 0
        lax.fori_loop(0, nt - 1, step, 0)

    def send_dp(copies):
        def one(p):
            for src_of, dst, s in copies:
                remote(src_of(p), dst, s, {"dp": p}).start()

        def step(j, _):
            one(dp_peer(nd, d, j))
            return 0
        lax.fori_loop(0, nd - 2, step, 0)
        one(d + 1 - 2 * (d % 2))

    def tp_wait(buf, s):
        return remote(buf.at[pl.ds(0, nt - 1)], buf.at[pl.ds(0, nt - 1)], s, {"tp": t})

    def dp_wait(buf, s):
        return remote(buf.at[pl.ds(0, nd - 1)], buf.at[pl.ds(0, nd - 1)], s, {"dp": d})

    row8 = lax.broadcasted_iota(jnp.int32, (sr, LN), 0)
    lane8 = lax.broadcasted_iota(jnp.int32, (sr, LN), 1)
    live = jnp.zeros((sr, LN), jnp.int32)
    for i in range(sr):
        live = jnp.where(row8 == i, lens[i], live)

    loads[0].wait()
    cur = x_v
    for l in range(2):
        q = 5 * l
        send_tp(lambda p: cur, xg.at[l, t], q)
        xg[l, t] = cur[...]
        if l == 0:
            for c in loads[1:]:
                c.wait()
        tp_wait(xg.at[l], q).wait_recv()
        xf = xg[l].reshape(nr, LN).astype(F32)
        scaled = (xf * gain_v[l][None, :]).astype(BF)
        part = jnp.dot(scaled, wcat[l], preferred_element_type=F32)
        pb[l] = part.reshape(nd, sr, 2 * LN).astype(BF)
        sq = xf * xf
        hi = sq.astype(BF)
        lo = (sq - hi.astype(F32)).astype(BF)
        ones = jnp.ones((8, LN), BF)
        dn = (((1,), (1,)), ((), ()))
        st = (lax.dot_general(ones, hi, dn, preferred_element_type=F32)
              + lax.dot_general(ones, lo, dn, preferred_element_type=F32))
        if nr < LN:
            st = jnp.concatenate([st, jnp.zeros((8, LN - nr), F32)], axis=1)
        for k in range(max(nr // LN, 1)):
            ssb[l, k] = st[0:1, k * LN:(k + 1) * LN]
        per = LN // sr
        send_dp([
            (lambda p: pb.at[l, p], rb.at[l, d], q + 1),
            (lambda p: ssb.at[l, p // per], ssr.at[l, d], q + 2),
        ])
        rb[l, d] = pb[l, d]
        ssr[l, d] = ssb[l, d // per]

        taps = cw_v[l].astype(F32)
        nt_taps = taps.shape[0] - 1
        past = jnp.zeros((sr, LN), F32)
        for back in range(1, nt_taps + 1):
            past = past + taps[nt_taps - back:nt_taps - back + 1] * jnp.where(
                live > back, cs_v[l, nt_taps - back].astype(F32), 0.0)
        previous = jnp.where(live > 1, rs_v[l], 0.0)
        soft = jax.nn.softplus(-dec_v[l:l + 1])

        dp_wait(rb.at[l], q + 1).wait_recv()
        dp_wait(ssr.at[l], q + 2).wait_recv()
        acc = jnp.sum(rb[l].astype(F32), axis=0)
        sst = jnp.sum(ssr[l], axis=0)
        ss = jnp.sum(jnp.where(lane8 == row8 + sr * (d % per), sst, 0.0), axis=1, keepdims=True)
        scale = lax.rsqrt(ss / width + EPS)
        value = acc[:, :LN] * scale
        gate = acc[:, LN:] * scale
        conv = taps[nt_taps:] * value + past
        gg = jax.nn.sigmoid(jnp.dot(conv.astype(BF), rcat[l], preferred_element_type=F32))
        log_decay = -8.0 * gg[:, :LN] * soft
        hidden = jnp.exp(log_decay) * previous + jnp.sqrt(one_less_exp(2.0 * log_decay)) * (
            gg[:, LN:] * conv)
        ro[l] = (hidden * jax.nn.gelu(gate)).astype(BF)
        send_dp([(lambda p: ro.at[l], rg.at[l, d], q + 3)])
        rg[l, d] = ro[l]
        for m in range(nt_taps - 1):
            nconv_v[l, m] = cs_v[l, m + 1]
        nconv_v[l, nt_taps - 1] = value.astype(BF)
        nrec_v[l] = hidden
        pltpu.make_async_copy(nconv_v.at[l], nconv.at[l], osem.at[0]).start()
        pltpu.make_async_copy(nrec_v.at[l], nrec.at[l], osem.at[1]).start()

        dp_wait(rg.at[l], q + 3).wait_recv()
        out = jnp.dot(rg[l].astype(F32).reshape(nr, LN).astype(BF), wout_v[l], preferred_element_type=F32)
        ob[l] = out.reshape(nt, tr, LN).astype(BF)
        send_tp(lambda p: ob.at[l, p], og.at[l, t], q + 4)
        og[l, t] = ob[l, t]
        tp_wait(og.at[l], q + 4).wait_recv()
        branch = jnp.sum(og[l].astype(F32), axis=0)
        x1[l] = (cur[...].astype(F32) + branch).astype(BF)
        cur = x1.at[l]

    last = pltpu.make_async_copy(x1.at[1], mixed, osem.at[2])
    last.start()
    for l in range(2):
        q = 5 * l
        tp_wait(xg.at[l], q).wait_send()
        dp_wait(rb.at[l], q + 1).wait_send()
        dp_wait(ssr.at[l], q + 2).wait_send()
        dp_wait(rg.at[l], q + 3).wait_send()
        tp_wait(og.at[l], q + 4).wait_send()
    pltpu.make_async_copy(nconv_v, nconv, osem.at[0]).wait()
    pltpu.make_async_copy(nrec_v, nrec, osem.at[1]).wait()
    last.wait()


def solution(mesh):
    nt, nd = mesh.shape["tp"], mesh.shape["dp"]

    def body(tokens, norm_gain, w_input, w_gate, w_recur, w_inject, conv_weight, decay_param,
             w_output, lengths, conv_state, rec_state):
        tr, sr = tokens.shape[0], lengths.shape[0]
        anyspec = pl.BlockSpec(memory_space=pl.ANY)
        V = pltpu.VMEM
        return pl.pallas_call(
            functools.partial(kernel, nt, nd, tr, sr),
            out_shape=(
                jax.ShapeDtypeStruct(tokens.shape, BF),
                jax.ShapeDtypeStruct(conv_state.shape, BF),
                jax.ShapeDtypeStruct(rec_state.shape, F32),
            ),
            in_specs=[pl.BlockSpec(memory_space=pltpu.SMEM)] + [anyspec] * 11,
            out_specs=(anyspec,) * 3,
            scratch_shapes=[
                V((tr, LN), BF), V((2, LN), F32), V((2, LN, 2 * LN), BF), V((2, LN, 2 * LN), BF),
                V(conv_weight.shape, BF), V((2, LN), F32), V((2, LN, LN), BF),
                V(conv_state.shape, BF), V(rec_state.shape, F32),
                V((2, nt, tr, LN), BF), V((2, nd, sr, 2 * LN), BF), V((2, nd, sr, 2 * LN), BF),
                V((2, max(nt * tr // LN, 1), 1, LN), F32), V((2, nd, 1, LN), F32),
                V((2, sr, LN), BF), V((2, nd, sr, LN), BF),
                V((2, nt, tr, LN), BF), V((2, nt, tr, LN), BF), V((2, tr, LN), BF),
                V(conv_state.shape, BF), V(rec_state.shape, F32),
                pltpu.SemaphoreType.DMA((10,)), pltpu.SemaphoreType.DMA((10,)),
                pltpu.SemaphoreType.DMA((11,)), pltpu.SemaphoreType.DMA((3,)),
            ],
            compiler_params=pltpu.CompilerParams(collective_id=0, has_side_effects=True),
        )(lengths, tokens, norm_gain, w_input, w_gate, w_recur, w_inject, conv_weight, decay_param,
          w_output, conv_state, rec_state)

    placed = (
        P("tp", "dp"),
        P(None, "dp"),
        P(None, "dp", "tp"),
        P(None, "dp", "tp"),
        P(None, "tp", None, None),
        P(None, "tp", None, None),
        P(None, None, "tp"),
        P(None, "tp"),
        P(None, "tp", "dp"),
        P("dp"),
        P(None, None, "dp", "tp"),
        P(None, "dp", "tp"),
    )
    return jax.shard_map(
        body,
        mesh=mesh,
        in_specs=placed,
        out_specs=(P("tp", "dp"), P(None, None, "dp", "tp"), P(None, "dp", "tp")),
        check_vma=False,
    )
```
